32 devices in a mesh: dp: 2 (over x), kv: 8 (over z, y), tp: 2 (over core).
Axes of the slice: x: 2, y: 2, z: 4, core: 2. Of those that a mesh axis runs over, the one named last changes fastest.
Arguments:
- tokens: bfloat16 [128, 4096], P('dp', 'kv'), may hold values from -6 to 6
- norm_gain: float32 [4096], P('kv'), may hold values from 0.1 to 1.9
- w_query: bfloat16 [4096, 2048], P('kv', 'tp'), may hold values from -0.09375 to 0.09375
- w_key: bfloat16 [4096, 2048], P('kv', 'tp'), may hold values from -0.09375 to 0.09375
- w_value: bfloat16 [4096, 2048], P('kv', 'tp'), may hold values from -0.09375 to 0.09375
- query_gain: float32 [64], replicated, may hold values from 0.1 to 1.9
- key_gain: float32 [64], replicated, may hold values from 0.1 to 1.9
- head_bias: float32 [32], P('tp'), may hold values from -11 to -3
- w_output: bfloat16 [2048, 4096], P('tp', 'kv'), may hold values from -0.125 to 0.125
- cache_keys: bfloat16 [8, 2048, 2048], P('dp', 'kv', 'tp'), may hold values from -6 to 6
- cache_values: bfloat16 [8, 2048, 2048], P('dp', 'kv', 'tp'), may hold values from -6 to 6
- base_length: int32 [8], P('dp'), may hold values from 1536 to 2016
- accepted: int32 [8], P('dp'), may hold values from 0 to 16
- parents: int32 [8, 16], P('dp'), may hold values from -1 to 14, as said below
Outputs:
- layer_out: bfloat16 [128, 4096], P('dp', 'kv')
- updated_keys: bfloat16 [8, 2048, 2048], P('dp', 'kv', 'tp')
- updated_values: bfloat16 [8, 2048, 2048], P('dp', 'kv', 'tp')
The draws below stay inside these ranges and needn't reach their ends.
Inputs may be any that keep to these rules, and one draw needn't show every extreme that they name: base_length + accepted + 16 <= 2048 for every sequence. parents[s, i] is -1 or a proposal before i; parents[s, 0] is -1.
All inputs are finite; a program needn't handle non-finite values.
Results may differ from the reference program's by a relative error of at most 0.00175.
The reference program's roundings to bfloat16 on the way count: a program that leaves them out, or rounds other values in their place, can miss the bound.
Values may be sent and summed in bfloat16 or wider, within the bound.
A program may use at most 64 MiB of HBM per device.

```python
import jax
import jax.numpy as jnp
from jax import lax

D = 4096
HEADS = 32
HEAD_DIM = 64
PROP = 16
CACHE_DEV = 256
SEQS = 8
CACHE = 2048
ROWS = 128
QW = 2048
N_KV = 8


def draw_head_bias(key, part):
    pick_key, slow_key, fast_key = jax.random.split(key, 3)
    slow = jax.random.uniform(pick_key, (HEADS,)) < 0.5
    slow_value = jax.random.uniform(slow_key, (HEADS,), jnp.float32, -11.0, -8.0)
    fast_value = jax.random.uniform(fast_key, (HEADS,), jnp.float32, -4.5, -3.0)
    return jnp.where(slow, slow_value, fast_value).astype(jnp.float32)


def draw_cache_values(key, part):
    centre_key, noise_key = jax.random.split(key)
    centre = jax.random.normal(centre_key, (SEQS, 1, HEADS * HEAD_DIM), jnp.float32)
    noise = 0.5 * jax.random.normal(noise_key, (SEQS, CACHE, HEADS * HEAD_DIM), jnp.float32)
    return jnp.clip(centre + noise, -6.0, 6.0).astype(jnp.bfloat16)


def draw_parents(key, part):
    step_back = jax.random.randint(key, (SEQS, PROP), 1, 4)
    column = jnp.arange(PROP, dtype=jnp.int32)[None, :]
    step_back = jnp.where(column == PROP - 1, 1, step_back).astype(jnp.int32)
    return jnp.maximum(column - step_back, -1).astype(jnp.int32)


def touch_ends(entries, key, smallest, largest):
    longest = entries.shape.index(max(entries.shape))
    spots = []
    for shift in (0, 1):
        where = [jax.random.randint(jax.random.fold_in(key, axis), (), 0, length) for axis, length in enumerate(entries.shape)]
        where[longest] = (where[longest] + shift) % entries.shape[longest]
        spots.append(tuple(where))
    return entries.at[spots[0]].set(smallest).at[spots[1]].set(largest)


def level_of(rng, dims, cuts, low, high):
    factor_of = 1.0
    for axis_at, parts in cuts:
        heights = jax.random.uniform(jax.random.fold_in(jax.random.fold_in(rng, 6), axis_at), (parts,), jnp.float32, low / len(cuts), high / len(cuts))
        factor_of = factor_of * jnp.repeat(jnp.exp(heights), dims[axis_at] // parts).reshape((-1,) + (1,) * (len(dims) - 1 - axis_at))
    return factor_of


def normal_values(rng, extent, scale, reach, pieces=(), kind=jnp.bfloat16):
    loudness = level_of(rng, extent, pieces, -0.22, 0.18) if pieces else 1.0
    array = jax.random.normal(rng, extent, jnp.float32) * scale * loudness
    return jnp.minimum(jnp.maximum(array, -reach), reach).astype(kind)


def setup_inputs(seed: int = 0) -> dict:
    streams_of = jax.random.split(jax.random.key(seed), 15)
    tokens = normal_values(streams_of[0], (ROWS, D), 1.0, 6.0, ((0, 2), (1, 8)))
    norm_gain = jnp.clip(1.0 + 0.18 * jax.random.normal(streams_of[1], (D,), jnp.float32), 0.1, 1.9)
    w_query = normal_values(streams_of[2], (D, QW), D ** -0.5, 0.09375, ((0, 8), (1, 2)))
    w_key = normal_values(streams_of[3], (D, QW), D ** -0.5, 0.09375, ((0, 8), (1, 2)))
    w_value = normal_values(streams_of[4], (D, QW), D ** -0.5, 0.09375, ((0, 8), (1, 2)))
    query_gain = jnp.clip(1.0 + 0.18 * jax.random.normal(streams_of[5], (HEAD_DIM,), jnp.float32), 0.1, 1.9)
    key_gain = jnp.clip(1.0 + 0.18 * jax.random.normal(streams_of[6], (HEAD_DIM,), jnp.float32), 0.1, 1.9)
    head_bias = draw_head_bias(jax.random.fold_in(streams_of[14], 71), 0)
    w_output = normal_values(streams_of[8], (QW, D), QW ** -0.5, 0.125, ((0, 2), (1, 8)))
    cache_keys = normal_values(streams_of[9], (SEQS, CACHE, QW), 1.0, 6.0, ((0, 2), (1, 8), (2, 2)))
    cache_values = draw_cache_values(jax.random.fold_in(streams_of[14], 71), 0)
    base_length = touch_ends(jax.random.randint(streams_of[11], (SEQS,), CACHE - CACHE // 4, CACHE - 2 * PROP + 1), jax.random.fold_in(streams_of[11], 1), CACHE - CACHE // 4, CACHE - 2 * PROP).astype(jnp.int32)
    accepted = touch_ends(jax.random.randint(streams_of[12], (SEQS,), 0, PROP + 1), jax.random.fold_in(streams_of[12], 1), 0, PROP).astype(jnp.int32)
    parents = draw_parents(jax.random.fold_in(streams_of[14], 71), 0)
    return dict(tokens=tokens, norm_gain=norm_gain, w_query=w_query, w_key=w_key, w_value=w_value, query_gain=query_gain, key_gain=key_gain, head_bias=head_bias, w_output=w_output, cache_keys=cache_keys, cache_values=cache_values, base_length=base_length, accepted=accepted, parents=parents)


epsilon = 1e-05

def head_norm(raw, gain):
    grouped = raw.reshape(raw.shape[0], -1, gain.shape[0])
    factor = lax.rsqrt(lax.optimization_barrier(jnp.mean(grouped * grouped, axis=2, keepdims=True)) + epsilon)
    return (grouped * factor * gain).reshape(raw.shape).astype(jnp.bfloat16)

def ancestry(parents):
    width = parents.shape[-1]
    direct = (parents[..., :, None] == jnp.arange(width, dtype=jnp.int32)).astype(jnp.float32)

    def extend(step, above):
        return direct + jnp.einsum('sij,sjk->sik', direct, above)
    return lax.fori_loop(0, width - 1, extend, direct)

def attend_one(head_bias, inputs):
    query_heads, key_heads, value_heads, stored_keys, stored_values, visible_len, tree = inputs
    factor = HEAD_DIM ** (-0.5)
    query_wide = query_heads.astype(jnp.float32)
    stored_k = stored_keys.astype(jnp.float32).reshape(CACHE, HEADS, HEAD_DIM)
    stored_v = stored_values.astype(jnp.float32).reshape(N_KV, CACHE_DEV, HEADS, HEAD_DIM)
    score = jnp.einsum('qhd,phd->hqp', query_wide, stored_k) * factor + head_bias[:, None, None]
    live = jnp.arange(CACHE, dtype=jnp.int32) < visible_len
    stay = jnp.where(live, jax.nn.log_sigmoid(-score), 0.0)
    stay_blocks = stay.reshape(HEADS, PROP, N_KV, CACHE_DEV)
    taken = jax.nn.log_sigmoid(score).reshape(HEADS, PROP, N_KV, CACHE_DEV)
    tail = lax.cumsum(stay_blocks, axis=3, reverse=True) - stay_blocks
    weight = jnp.where(live.reshape(N_KV, CACHE_DEV), jnp.exp(taken + tail), 0.0).astype(jnp.bfloat16)
    block_sum = jnp.einsum('hqbc,bchd->qbhd', weight.astype(jnp.float32), stored_v)
    block_log = lax.optimization_barrier(jnp.sum(stay_blocks, axis=3))
    later = lax.cumsum(block_log, axis=2, reverse=True) - block_log
    cache_part = jnp.einsum('hqb,qbhd->qhd', jnp.exp(later), block_sum)
    inner = jnp.einsum('qhd,jhd->hqj', query_wide, key_heads.astype(jnp.float32)) * factor + head_bias[:, None, None]
    mine = tree > 0.5
    stay_tree = jnp.where(mine, jax.nn.log_sigmoid(-inner), 0.0)
    tail_tree = lax.cumsum(stay_tree, axis=2, reverse=True) - stay_tree
    weight_tree = jnp.where(mine, jnp.exp(jax.nn.log_sigmoid(inner) + tail_tree), 0.0).astype(jnp.bfloat16)
    ancestor_sum = jnp.einsum('hqj,jhd->qhd', weight_tree.astype(jnp.float32), value_heads.astype(jnp.float32))
    ancestor_log = lax.optimization_barrier(jnp.sum(stay_tree, axis=2))
    total = ancestor_sum + jnp.exp(ancestor_log).T[:, :, None] * cache_part
    return total.reshape(PROP, HEADS * HEAD_DIM)

def reference(tokens, norm_gain, w_query, w_key, w_value, query_gain, key_gain, head_bias, w_output, cache_keys, cache_values, base_length, accepted, parents):
    wide = tokens.astype(jnp.float32)
    scaled = (wide * norm_gain).astype(jnp.bfloat16)
    inv_rms = lax.rsqrt(lax.optimization_barrier(jnp.mean(wide * wide, axis=1)) + epsilon)
    query_raw = jnp.dot(scaled, w_query, preferred_element_type=jnp.float32)
    key_raw = jnp.dot(scaled, w_key, preferred_element_type=jnp.float32)
    value_raw = jnp.dot(scaled, w_value, preferred_element_type=jnp.float32)
    queries = head_norm(query_raw, query_gain)
    new_keys = head_norm(key_raw, key_gain)
    new_values = (value_raw * inv_rms[:, None]).astype(jnp.bfloat16)
    valid = (base_length + accepted).astype(jnp.int32)
    tree = ancestry(parents)
    seq_count = cache_keys.shape[0]
    shape_four = (seq_count, PROP, HEADS, HEAD_DIM)
    attended = lax.map(partial_attend(head_bias), (queries.reshape(shape_four), new_keys.reshape(shape_four), new_values.reshape(shape_four), cache_keys, cache_values, valid, tree))
    attended = attended.reshape(seq_count * PROP, HEADS * HEAD_DIM).astype(jnp.bfloat16)
    mix = jnp.dot(attended, w_output, preferred_element_type=jnp.float32)
    layer_out = (mix * lax.rsqrt(lax.optimization_barrier(jnp.mean(mix * mix, axis=1, keepdims=True)) + epsilon)).astype(jnp.bfloat16)

    def write(stored, fresh, start):
        return lax.dynamic_update_slice_in_dim(stored, fresh, start, axis=0)
    updated_keys = jax.vmap(write)(cache_keys, new_keys.reshape(seq_count, PROP, -1), valid)
    updated_values = jax.vmap(write)(cache_values, new_values.reshape(seq_count, PROP, -1), valid)
    return (layer_out, updated_keys, updated_values)

def partial_attend(head_bias):

    def apply(inputs):
        return attend_one(head_bias, inputs)
    return apply
```

```python
import functools

import jax
import jax.numpy as jnp
from jax import lax
from jax.experimental import pallas as pl
from jax.experimental.pallas import tpu as pltpu
from jax.sharding import PartitionSpec as P

D = 4096
HEAD_DIM = 64
epsilon = 1e-05
MESH = pl.DeviceIdType.MESH
F32 = jnp.float32
BF16 = jnp.bfloat16


def iota(shape, axis):
    return lax.broadcasted_iota(jnp.int32, shape, axis)


def dot(a, b):
    return jnp.dot(a, b, preferred_element_type=F32)


def dot_t(a, b):
    return lax.dot_general(a, b, (((1,), (1,)), ((), ())), preferred_element_type=F32)


def exact_dot(a, ones):
    high = a.astype(BF16)
    rest = a - high.astype(F32)
    middle = rest.astype(BF16)
    low = (rest - middle.astype(F32)).astype(BF16)
    return dot(high, ones) + dot(middle, ones) + dot(low, ones)


def pack(rows):
    block = jnp.bitwise_and(iota((8, rows.shape[1]), 1), HEAD_DIM - 1) >> 3
    out = jnp.zeros((8, rows.shape[1]), F32)
    for j in range(rows.shape[0] // 8):
        out = jnp.where(block == j, rows[8 * j : 8 * j + 8], out)
    return out


def spread(packed, rows):
    inner = jnp.bitwise_and(iota(packed.shape, 1), HEAD_DIM - 1)
    return jnp.concatenate(
        [jnp.where(inner == 8 * j, packed, 0.0) for j in range(rows // 8)], axis=0
    )


def unpack_column(packed, rows):
    wide = spread(packed, rows)
    return jnp.sum(jnp.where(iota(wide.shape, 1) < HEAD_DIM, wide, 0.0), axis=1, keepdims=True)


def per_head(columns, width):
    lane_head = iota((columns[0].shape[0], width), 1) // HEAD_DIM
    out = jnp.broadcast_to(columns[0], lane_head.shape)
    for h in range(1, len(columns)):
        out = jnp.where(lane_head == h, columns[h], out)
    return out


def soft_stay(score):
    return -(jnp.maximum(score, 0.0) + jnp.log1p(jnp.exp(-jnp.abs(score))))


def greet(peers):
    barrier = pltpu.get_barrier_semaphore()
    for where in peers:
        pl.semaphore_signal(barrier, inc=1, device_id=where, device_id_type=MESH)
    pl.semaphore_wait(barrier, len(peers))


def head_norm(raw, gain):
    width = raw.shape[1]
    lane_head = iota(raw.shape, 1) // HEAD_DIM
    square = raw * raw
    means = [
        jnp.sum(jnp.where(lane_head == h, square, 0.0), axis=1, keepdims=True) / HEAD_DIM
        for h in range(width // HEAD_DIM)
    ]
    factor = per_head([lax.rsqrt(m + epsilon) for m in means], width)
    return (raw * factor * gain).astype(BF16)


def project_kernel(
    n,
    width,
    tokens_ref,
    norm_ref,
    wq_hbm,
    wk_hbm,
    wv_hbm,
    qgain_ref,
    kgain_ref,
    bias_ref,
    parents_ref,
    q_out,
    k_out,
    v_out,
    tree_sum_out,
    tree_exp_out,
    wq,
    wk,
    wv,
    send,
    recv,
    mine,
    gath,
    load_sem,
    send_sem,
    recv_sem,
    gsend_sem,
    grecv_sem,
):
    me = lax.axis_index("kv")
    loads = [
        pltpu.make_async_copy(a, b, load_sem.at[i])
        for i, (a, b) in enumerate(((wq_hbm, wq), (wk_hbm, wk), (wv_hbm, wv)))
    ]
    for load in loads:
        load.start()
    greet([{"kv": lax.rem(me + d, n)} for d in range(1, n)])
    rows = tokens_ref.shape[0]
    w = send.shape[2]
    wide = tokens_ref[...].astype(F32)
    scaled = (wide * norm_ref[...]).astype(BF16)
    squares = jnp.sum(wide * wide, axis=1, keepdims=True)
    squares = pack(jnp.broadcast_to(squares, (rows, w)))
    for load in loads:
        load.wait()

    def scatter(p):
        return pltpu.make_async_remote_copy(
            src_ref=send.at[p],
            dst_ref=recv.at[me],
            send_sem=send_sem.at[p],
            recv_sem=recv_sem.at[me],
            device_id={"kv": p},
            device_id_type=MESH,
        )

    total = n * w
    chunk = 256
    for c in range(0, total, chunk):
        for i, weight in enumerate((wq, wk, wv)):
            part = dot(scaled, weight[:, c : c + chunk])
            for p in range(c // w, (c + chunk) // w):
                send[p, i * rows : (i + 1) * rows, :] = part[:, p * w - c : (p + 1) * w - c]
        for p in range(c // w, (c + chunk) // w):
            send[p, 3 * rows :, :] = squares

            @pl.when(p != me)
            def _():
                scatter(p).start()

    owner = iota((rows, rows), 0) // width
    column = iota((rows, rows), 1)
    parents = parents_ref[...]
    direct = (column - owner * width == parents) & (column // width == owner)
    step = jnp.where(direct, 1.0, 0.0)
    reach = step
    span = 1
    while span < width:
        reach = reach + dot(reach.astype(BF16), step.astype(BF16))
        step = dot(step.astype(BF16), step.astype(BF16))
        span *= 2

    def from_peer(buffer, sem, ssem, source):
        return pltpu.make_async_remote_copy(
            src_ref=buffer.at[source],
            dst_ref=buffer.at[source],
            send_sem=ssem.at[source],
            recv_sem=sem.at[source],
            device_id={"kv": source},
            device_id_type=MESH,
        )

    summed = send[me]
    for d in range(1, n):
        source = lax.rem(me + d, n)
        from_peer(recv, recv_sem, send_sem, source).wait_recv()
        summed = summed + recv[source]
    query_raw = summed[:rows]
    key_raw = summed[rows : 2 * rows]
    value_raw = summed[2 * rows : 3 * rows]
    inv_rms = lax.rsqrt(unpack_column(summed[3 * rows :], rows) / D + epsilon)
    queries = head_norm(query_raw, qgain_ref[...])
    new_keys = head_norm(key_raw, kgain_ref[...])
    new_values = (value_raw * inv_rms).astype(BF16)
    mine[0:rows, :] = queries
    mine[rows : 2 * rows, :] = new_keys
    mine[2 * rows : 3 * rows, :] = new_values

    def spread_out(p):
        return pltpu.make_async_remote_copy(
            src_ref=mine,
            dst_ref=gath.at[me],
            send_sem=gsend_sem.at[p],
            recv_sem=grecv_sem.at[me],
            device_id={"kv": p},
            device_id_type=MESH,
        )

    for d in range(1, n):
        spread_out(lax.rem(me + d, n)).start()
    gath[me] = mine[...]

    heads = w // HEAD_DIM
    lane_head = iota((rows, w), 1) // HEAD_DIM
    sums, exps = [], []
    tri = jnp.where(iota((rows, rows), 0) > iota((rows, rows), 1), 1.0, 0.0).astype(BF16)
    mask = reach > 0.5
    for h in range(heads):
        only = jnp.where(lane_head == h, queries.astype(F32), 0.0).astype(BF16)
        score = dot_t(only, new_keys) * (HEAD_DIM ** (-0.5))
        score = score + bias_ref[0:1, h : h + 1]
        stay = soft_stay(score)
        taken = score + stay
        stay = jnp.where(mask, stay, 0.0)
        tail = exact_dot(stay, tri)
        weight = jnp.where(mask, jnp.exp(taken + tail), 0.0).astype(BF16)
        sums.append(dot(weight, new_values))
        exps.append(jnp.exp(jnp.sum(stay, axis=1, keepdims=True)))
    tree_sum = sums[0]
    for h in range(1, heads):
        tree_sum = jnp.where(lane_head == h, sums[h], tree_sum)
    tree_sum_out[...] = tree_sum
    tree_exp_out[...] = per_head(exps, w)

    for p in range(n):

        @pl.when(p != me)
        def _():
            from_peer(gath, grecv_sem, gsend_sem, p).wait_recv()

        q_out[:, p * w : (p + 1) * w] = gath[p, 0:rows, :]
        k_out[:, p * w : (p + 1) * w] = gath[p, rows : 2 * rows, :]
        v_out[:, p * w : (p + 1) * w] = gath[p, 2 * rows : 3 * rows, :]
    for d in range(1, n):
        peer = lax.rem(me + d, n)
        scatter(peer).wait_send()
        spread_out(peer).wait_send()


def cache_kernel(
    n,
    width,
    base_ref,
    accepted_ref,
    bias_ref,
    q_ref,
    k_ref,
    v_ref,
    ck_ref,
    cv_ref,
    pay_ref,
    uk_ref,
    uv_ref,
):
    me = lax.axis_index("kv")
    s = pl.program_id(0)
    span = ck_ref.shape[1]
    total = ck_ref.shape[2]
    w = pay_ref.shape[2]
    rows = pay_ref.shape[1] - 8
    valid = base_ref[s] + accepted_ref[s]
    start = me * span
    group = 256
    heads = group // HEAD_DIM
    own = iota((heads * width, group), 0) // width == iota((heads * width, group), 1) // HEAD_DIM
    scores = []
    for c in range(0, total, group):
        q = q_ref[:, c : c + group].astype(F32)
        diagonal = jnp.where(own, jnp.concatenate([q] * heads, axis=0), 0.0).astype(BF16)
        scores.append(dot_t(diagonal, ck_ref[0, :, c : c + group]))
    score = jnp.concatenate(scores, axis=0) * (HEAD_DIM ** (-0.5)) + bias_ref[...]
    live = start + iota(score.shape, 1) < valid
    stay = soft_stay(score)
    taken = score + stay
    stay = jnp.where(live, stay, 0.0)
    tri = jnp.where(iota((span, span), 0) > iota((span, span), 1), 1.0, 0.0).astype(BF16)
    tail = exact_dot(stay, tri)
    weight = jnp.where(live, jnp.exp(taken + tail), 0.0).astype(BF16)
    logs = jnp.sum(stay, axis=1, keepdims=True)
    at = pl.multiple_of(s * width, width)
    for g, c in enumerate(range(0, total, group)):
        r = slice(g * heads * width, (g + 1) * heads * width)
        full = jnp.where(own, dot(weight[r], cv_ref[0, :, c : c + group]), 0.0)
        log_full = jnp.where(own, logs[r], 0.0)
        block = full[0:width]
        log_block = log_full[0:width]
        for h in range(1, heads):
            block = block + full[h * width : (h + 1) * width]
            log_block = log_block + log_full[h * width : (h + 1) * width]
        for p in range(c // w, (c + group) // w):
            lanes = slice(p * w - c, (p + 1) * w - c)
            pay_ref[p, pl.ds(at, width), :] = block[:, lanes]
            slot = jnp.bitwise_and(iota((8, w), 1), HEAD_DIM - 1) >> 3
            packed = jnp.where(s == 0, jnp.zeros((8, w), F32), pay_ref[p, rows : rows + 8, :])
            for j in range(width // 8):
                packed = jnp.where(
                    slot == s * (width // 8) + j, log_block[8 * j : 8 * j + 8, lanes], packed
                )
            pay_ref[p, rows : rows + 8, :] = packed
    uk_ref[...] = ck_ref[...]
    uv_ref[...] = cv_ref[...]

    @pl.when((valid + width > start) & (valid < start + span))
    def _():
        offset = start + iota((span, width), 0) - valid
        chooser = jnp.where(offset == iota((span, width), 1), 1.0, 0.0).astype(BF16)
        offset = start + iota((span, total), 0) - valid
        inside = (offset >= 0) & (offset < width)
        for fresh, old, out in ((k_ref, ck_ref, uk_ref), (v_ref, cv_ref, uv_ref)):
            placed = dot(chooser, fresh[...])
            out[0] = jnp.where(inside, placed, old[0].astype(F32)).astype(BF16)


def output_kernel(
    n,
    pay_ref,
    tree_sum_ref,
    tree_exp_ref,
    wo_hbm,
    out_ref,
    wo,
    recv,
    att,
    gath,
    wide,
    part,
    other,
    sq,
    sqs,
    load_sem,
    send_sem,
    recv_sem,
    gsend_sem,
    grecv_sem,
    pair_sem,
    ssend_sem,
    srecv_sem,
):
    me = lax.axis_index("kv")
    core = lax.axis_index("tp")
    cores = lax.axis_size("tp")
    load = pltpu.make_async_copy(wo_hbm, wo, load_sem)
    load.start()
    peers = [lax.rem(me + d, n) for d in range(1, n)]
    partners = [lax.rem(core + d, cores) for d in range(1, cores)]
    greet([{"kv": p} for p in peers] + [{"tp": t} for t in partners])

    def push(src, dst, ssem, rsem, p):
        return pltpu.make_async_remote_copy(
            src_ref=src,
            dst_ref=dst.at[me],
            send_sem=ssem.at[p],
            recv_sem=rsem.at[me],
            device_id={"kv": p},
            device_id_type=MESH,
        )

    def arrived(dst, ssem, rsem, p):
        pltpu.make_async_remote_copy(
            src_ref=dst.at[p],
            dst_ref=dst.at[p],
            send_sem=ssem.at[p],
            recv_sem=rsem.at[p],
            device_id={"kv": p},
            device_id_type=MESH,
        ).wait_recv()

    for p in peers:
        push(pay_ref.at[p], recv, send_sem, recv_sem, p).start()
    recv[me] = pay_ref[me]
    rows, w = att.shape
    for p in peers:
        arrived(recv, send_sem, recv_sem, p)
    later = jnp.zeros((8, w), F32)
    scales = [None] * n
    for b in range(n - 1, -1, -1):
        scales[b] = spread(jnp.exp(later), rows)
        later = later + recv[b, rows : rows + 8, :]
    same = iota((w, w), 0) // HEAD_DIM == iota((w, w), 1) // HEAD_DIM
    same = jnp.where(same, 1.0, 0.0).astype(BF16)
    scale = exact_dot(jnp.concatenate(scales, axis=0), same)
    cache_part = jnp.zeros((rows, w), F32)
    for b in range(n):
        cache_part = cache_part + scale[b * rows : (b + 1) * rows] * recv[b, 0:rows, :]
    attended = tree_sum_ref[...] + tree_exp_ref[...] * cache_part
    att[...] = attended.astype(BF16)
    for p in peers:
        push(att, gath, gsend_sem, grecv_sem, p).start()
    gath[me] = att[...]
    load.wait()
    for p in range(n):

        @pl.when(p != me)
        def _():
            arrived(gath, gsend_sem, grecv_sem, p)

        wide[:, p * w : (p + 1) * w] = gath[p]
    part[...] = dot(wide[...], wo[...])
    swaps = [
        pltpu.make_async_remote_copy(
            src_ref=part,
            dst_ref=other.at[d],
            send_sem=pair_sem.at[0, d],
            recv_sem=pair_sem.at[1, d],
            device_id={"tp": t},
            device_id_type=MESH,
        )
        for d, t in enumerate(partners)
    ]
    for swap in swaps:
        swap.start()
    mix = part[...]
    for d, swap in enumerate(swaps):
        swap.wait_recv()
        mix = mix + other[d]
    squares = jnp.sum(mix * mix, axis=1, keepdims=True)
    sq[...] = pack(jnp.broadcast_to(squares, (rows, 128)))
    for p in peers:
        push(sq, sqs, ssend_sem, srecv_sem, p).start()
    sqs[me] = sq[...]
    for p in peers:
        arrived(sqs, ssend_sem, srecv_sem, p)
    total = sqs[0]
    for b in range(1, n):
        total = total + sqs[b]
    inv = lax.rsqrt(unpack_column(total, rows) / D + epsilon)
    out_ref[...] = (mix * inv).astype(BF16)
    for p in peers:
        push(pay_ref.at[p], recv, send_sem, recv_sem, p).wait_send()
        push(att, gath, gsend_sem, grecv_sem, p).wait_send()
        push(sq, sqs, ssend_sem, srecv_sem, p).wait_send()
    for swap in swaps:
        swap.wait_send()


def shards(
    n,
    tokens,
    norm_gain,
    w_query,
    w_key,
    w_value,
    query_gain,
    key_gain,
    head_bias,
    w_output,
    cache_keys,
    cache_values,
    base_length,
    accepted,
    parents,
):
    rows, depth = tokens.shape
    total = w_query.shape[1]
    w = total // n
    heads = w // HEAD_DIM
    seqs, width = parents.shape
    span = cache_keys.shape[1]
    columns = w_output.shape[1]
    vmem = pl.BlockSpec(memory_space=pltpu.VMEM)
    smem = pl.BlockSpec(memory_space=pltpu.SMEM)
    hbm = pl.BlockSpec(memory_space=pl.ANY)
    dma = pltpu.SemaphoreType.DMA
    mine_at = lax.axis_index("kv") * heads
    my_bias = lax.dynamic_slice(head_bias, (mine_at,), (heads,)).reshape(1, heads)
    queries, new_keys, new_values, tree_sum, tree_exp = pl.pallas_call(
        functools.partial(project_kernel, n, width),
        name="project",
        out_shape=[jax.ShapeDtypeStruct((rows, total), BF16)] * 3
        + [jax.ShapeDtypeStruct((rows, w), F32)] * 2,
        in_specs=[vmem, vmem, hbm, hbm, hbm, vmem, vmem, vmem, vmem],
        out_specs=[vmem] * 5,
        scratch_shapes=[
            pltpu.VMEM((depth, total), BF16),
            pltpu.VMEM((depth, total), BF16),
            pltpu.VMEM((depth, total), BF16),
            pltpu.VMEM((n, 3 * rows + 8, w), F32),
            pltpu.VMEM((n, 3 * rows + 8, w), F32),
            pltpu.VMEM((3 * rows, w), BF16),
            pltpu.VMEM((n, 3 * rows, w), BF16),
            dma((3,)),
            dma((n,)),
            dma((n,)),
            dma((n,)),
            dma((n,)),
        ],
        compiler_params=pltpu.CompilerParams(
            collective_id=0, has_side_effects=True, vmem_limit_bytes=32 * 2**20
        ),
    )(
        tokens,
        norm_gain.reshape(1, depth),
        w_query,
        w_key,
        w_value,
        jnp.tile(query_gain, heads).reshape(1, w),
        jnp.tile(key_gain, heads).reshape(1, w),
        my_bias,
        parents.reshape(rows, 1),
    )
    block = pl.BlockSpec((1, span, total), lambda s: (s, 0, 0))
    fresh = pl.BlockSpec((width, total), lambda s: (s, 0))
    pay, updated_keys, updated_values = pl.pallas_call(
        functools.partial(cache_kernel, n, width),
        name="cache",
        grid=(seqs,),
        out_shape=[
            jax.ShapeDtypeStruct((n, rows + 8, w), F32),
            jax.ShapeDtypeStruct(cache_keys.shape, BF16),
            jax.ShapeDtypeStruct(cache_values.shape, BF16),
        ],
        in_specs=[
            smem,
            smem,
            pl.BlockSpec((total // HEAD_DIM * width, 1), lambda s: (0, 0)),
            fresh,
            fresh,
            fresh,
            block,
            block,
        ],
        out_specs=[pl.BlockSpec((n, rows + 8, w), lambda s: (0, 0, 0)), block, block],
        compiler_params=pltpu.CompilerParams(
            dimension_semantics=("arbitrary",), vmem_limit_bytes=32 * 2**20
        ),
    )(
        base_length,
        accepted,
        jnp.repeat(head_bias, width).reshape(-1, 1),
        queries,
        new_keys,
        new_values,
        cache_keys,
        cache_values,
    )
    layer_out = pl.pallas_call(
        functools.partial(output_kernel, n),
        name="output",
        out_shape=jax.ShapeDtypeStruct((rows, columns), BF16),
        in_specs=[vmem, vmem, vmem, hbm],
        out_specs=vmem,
        scratch_shapes=[
            pltpu.VMEM(w_output.shape, BF16),
            pltpu.VMEM((n, rows + 8, w), F32),
            pltpu.VMEM((rows, w), BF16),
            pltpu.VMEM((n, rows, w), BF16),
            pltpu.VMEM((rows, total), BF16),
            pltpu.VMEM((rows, columns), F32),
            pltpu.VMEM((1, rows, columns), F32),
            pltpu.VMEM((8, 128), F32),
            pltpu.VMEM((n, 8, 128), F32),
            dma,
            dma((n,)),
            dma((n,)),
            dma((n,)),
            dma((n,)),
            dma((2, 1)),
            dma((n,)),
            dma((n,)),
        ],
        compiler_params=pltpu.CompilerParams(
            collective_id=1, has_side_effects=True, vmem_limit_bytes=32 * 2**20
        ),
    )(pay, tree_sum, tree_exp, w_output)
    return layer_out, updated_keys, updated_values


def solution(mesh):
    return jax.shard_map(
        functools.partial(shards, mesh.shape["kv"]),
        mesh=mesh,
        in_specs=(
            P("dp", "kv"),
            P("kv"),
            P("kv", "tp"),
            P("kv", "tp"),
            P("kv", "tp"),
            P(),
            P(),
            P("tp"),
            P("tp", "kv"),
            P("dp", "kv", "tp"),
            P("dp", "kv", "tp"),
            P("dp"),
            P("dp"),
            P("dp", None),
        ),
        out_specs=(P("dp", "kv"), P("dp", "kv", "tp"), P("dp", "kv", "tp")),
        check_vma=False,
    )
```

```python
import functools

import jax
import jax.numpy as jnp
from jax import lax
from jax.experimental import pallas as pl
from jax.experimental.pallas import tpu as pltpu
from jax.sharding import PartitionSpec as P

D = 4096
HEAD_DIM = 64
epsilon = 1e-05
MESH = pl.DeviceIdType.MESH
F32 = jnp.float32
BF16 = jnp.bfloat16


def iota(shape, axis):
    return lax.broadcasted_iota(jnp.int32, shape, axis)


def dot(a, b):
    return jnp.dot(a, b, preferred_element_type=F32)


def dot_t(a, b):
    return lax.dot_general(a, b, (((1,), (1,)), ((), ())), preferred_element_type=F32)


def exact_dot(a, ones):
    high = a.astype(BF16)
    rest = a - high.astype(F32)
    middle = rest.astype(BF16)
    low = (rest - middle.astype(F32)).astype(BF16)
    return dot(high, ones) + dot(middle, ones) + dot(low, ones)


def pack(rows):
    block = jnp.bitwise_and(iota((8, rows.shape[1]), 1), HEAD_DIM - 1) >> 3
    out = jnp.zeros((8, rows.shape[1]), F32)
    for j in range(rows.shape[0] // 8):
        out = jnp.where(block == j, rows[8 * j : 8 * j + 8], out)
    return out


def spread(packed, rows):
    inner = jnp.bitwise_and(iota(packed.shape, 1), HEAD_DIM - 1)
    return jnp.concatenate(
        [jnp.where(inner == 8 * j, packed, 0.0) for j in range(rows // 8)], axis=0
    )


def unpack_column(packed, rows):
    wide = spread(packed, rows)
    return jnp.sum(jnp.where(iota(wide.shape, 1) < HEAD_DIM, wide, 0.0), axis=1, keepdims=True)


def per_head(columns, width):
    lane_head = iota((columns[0].shape[0], width), 1) // HEAD_DIM
    out = jnp.broadcast_to(columns[0], lane_head.shape)
    for h in range(1, len(columns)):
        out = jnp.where(lane_head == h, columns[h], out)
    return out


def soft_stay(score):
    return -(jnp.maximum(score, 0.0) + jnp.log1p(jnp.exp(-jnp.abs(score))))


def greet(peers):
    barrier = pltpu.get_barrier_semaphore()
    for where in peers:
        pl.semaphore_signal(barrier, inc=1, device_id=where, device_id_type=MESH)
    pl.semaphore_wait(barrier, len(peers))


def head_norm(raw, gain):
    width = raw.shape[1]
    lane_head = iota(raw.shape, 1) // HEAD_DIM
    square = raw * raw
    means = [
        jnp.sum(jnp.where(lane_head == h, square, 0.0), axis=1, keepdims=True) / HEAD_DIM
        for h in range(width // HEAD_DIM)
    ]
    factor = per_head([lax.rsqrt(m + epsilon) for m in means], width)
    return (raw * factor * gain).astype(BF16)


def project_kernel(
    n,
    width,
    tokens_ref,
    norm_ref,
    wq_hbm,
    wk_hbm,
    wv_hbm,
    qgain_ref,
    kgain_ref,
    bias_ref,
    parents_ref,
    q_out,
    k_out,
    v_out,
    tree_sum_out,
    tree_exp_out,
    wq,
    wk,
    wv,
    send,
    half,
    pairs,
    recv,
    mine,
    gath,
    load_sem,
    hsend_sem,
    hrecv_sem,
    send_sem,
    recv_sem,
    gsend_sem,
    grecv_sem,
):
    me = lax.axis_index("kv")
    side = lax.rem(me, 2)
    spot = me // 2
    loads = [
        pltpu.make_async_copy(a, b, load_sem.at[i])
        for i, (a, b) in enumerate(((wq_hbm, wq), (wk_hbm, wk), (wv_hbm, wv)))
    ]
    for load in loads:
        load.start()
    greet([{"kv": lax.rem(me + d, n)} for d in range(1, n)])
    rows = tokens_ref.shape[0]
    w = send.shape[2]
    wide = tokens_ref[...].astype(F32)
    scaled = (wide * norm_ref[...]).astype(BF16)
    squares = jnp.sum(wide * wide, axis=1, keepdims=True)
    squares = pack(jnp.broadcast_to(squares, (rows, w)))
    for load in loads:
        load.wait()

    def to_pair(g):
        return pltpu.make_async_remote_copy(
            src_ref=send.at[2 * g + 1 - side],
            dst_ref=half.at[g],
            send_sem=hsend_sem.at[g],
            recv_sem=hrecv_sem.at[g],
            device_id={"kv": me + 1 - 2 * side},
            device_id_type=MESH,
        )

    def scatter(g):
        return pltpu.make_async_remote_copy(
            src_ref=pairs.at[g],
            dst_ref=recv.at[spot],
            send_sem=send_sem.at[g],
            recv_sem=recv_sem.at[spot],
            device_id={"kv": 2 * g + side},
            device_id_type=MESH,
        )

    total = n * w
    chunk = 256
    for c in range(0, total, chunk):
        for i, weight in enumerate((wq, wk, wv)):
            part = dot(scaled, weight[:, c : c + chunk])
            for p in range(c // w, (c + chunk) // w):
                send[p, i * rows : (i + 1) * rows, :] = part[:, p * w - c : (p + 1) * w - c]
        for p in range(c // w, (c + chunk) // w):
            send[p, 3 * rows :, :] = squares
        for g in range(c // w // 2, (c + chunk) // w // 2):
            to_pair(g).start()
    for g in range(n // 2):
        to_pair(g).wait_recv()
        pairs[g] = send[2 * g + side] + half[g]

        @pl.when(g != spot)
        def _():
            scatter(g).start()

    owner = iota((rows, rows), 0) // width
    column = iota((rows, rows), 1)
    parents = parents_ref[...]
    direct = (column - owner * width == parents) & (column // width == owner)
    step = jnp.where(direct, 1.0, 0.0)
    reach = step
    span = 1
    while span < width:
        reach = reach + dot(reach.astype(BF16), step.astype(BF16))
        step = dot(step.astype(BF16), step.astype(BF16))
        span *= 2

    def from_peer(buffer, sem, ssem, source):
        return pltpu.make_async_remote_copy(
            src_ref=buffer.at[source],
            dst_ref=buffer.at[source],
            send_sem=ssem.at[source],
            recv_sem=sem.at[source],
            device_id={"kv": source},
            device_id_type=MESH,
        )

    summed = pairs[spot]
    for d in range(1, n // 2):
        source = lax.rem(spot + d, n // 2)
        pltpu.make_async_remote_copy(
            src_ref=pairs.at[source],
            dst_ref=recv.at[source],
            send_sem=send_sem.at[source],
            recv_sem=recv_sem.at[source],
            device_id={"kv": 2 * source + side},
            device_id_type=MESH,
        ).wait_recv()
        summed = summed + recv[source]
    query_raw = summed[:rows]
    key_raw = summed[rows : 2 * rows]
    value_raw = summed[2 * rows : 3 * rows]
    inv_rms = lax.rsqrt(unpack_column(summed[3 * rows :], rows) / D + epsilon)
    queries = head_norm(query_raw, qgain_ref[...])
    new_keys = head_norm(key_raw, kgain_ref[...])
    new_values = (value_raw * inv_rms).astype(BF16)
    mine[0:rows, :] = queries
    mine[rows : 2 * rows, :] = new_keys
    mine[2 * rows : 3 * rows, :] = new_values

    def spread_out(p):
        return pltpu.make_async_remote_copy(
            src_ref=mine,
            dst_ref=gath.at[me],
            send_sem=gsend_sem.at[p],
            recv_sem=grecv_sem.at[me],
            device_id={"kv": p},
            device_id_type=MESH,
        )

    for d in range(1, n):
        spread_out(lax.rem(me + d, n)).start()
    gath[me] = mine[...]

    heads = w // HEAD_DIM
    lane_head = iota((rows, w), 1) // HEAD_DIM
    sums, exps = [], []
    tri = jnp.where(iota((rows, rows), 0) > iota((rows, rows), 1), 1.0, 0.0).astype(BF16)
    mask = reach > 0.5
    for h in range(heads):
        only = jnp.where(lane_head == h, queries.astype(F32), 0.0).astype(BF16)
        score = dot_t(only, new_keys) * (HEAD_DIM ** (-0.5))
        score = score + bias_ref[0:1, h : h + 1]
        stay = soft_stay(score)
        taken = score + stay
        stay = jnp.where(mask, stay, 0.0)
        tail = exact_dot(stay, tri)
        weight = jnp.where(mask, jnp.exp(taken + tail), 0.0).astype(BF16)
        sums.append(dot(weight, new_values))
        exps.append(jnp.exp(jnp.sum(stay, axis=1, keepdims=True)))
    tree_sum = sums[0]
    for h in range(1, heads):
        tree_sum = jnp.where(lane_head == h, sums[h], tree_sum)
    tree_sum_out[...] = tree_sum
    tree_exp_out[...] = per_head(exps, w)

    for p in range(n):

        @pl.when(p != me)
        def _():
            from_peer(gath, grecv_sem, gsend_sem, p).wait_recv()

        q_out[:, p * w : (p + 1) * w] = gath[p, 0:rows, :]
        k_out[:, p * w : (p + 1) * w] = gath[p, rows : 2 * rows, :]
        v_out[:, p * w : (p + 1) * w] = gath[p, 2 * rows : 3 * rows, :]
    for d in range(1, n):
        peer = lax.rem(me + d, n)
        spread_out(peer).wait_send()
    for d in range(1, n // 2):
        scatter(lax.rem(spot + d, n // 2)).wait_send()
    for g in range(n // 2):
        to_pair(g).wait_send()


def cache_kernel(
    n,
    width,
    base_ref,
    accepted_ref,
    bias_ref,
    q_ref,
    k_ref,
    v_ref,
    ck_ref,
    cv_ref,
    pay_ref,
    uk_ref,
    uv_ref,
):
    me = lax.axis_index("kv")
    s = pl.program_id(0)
    span = ck_ref.shape[1]
    total = ck_ref.shape[2]
    w = pay_ref.shape[2]
    rows = pay_ref.shape[1] - 8
    valid = base_ref[s] + accepted_ref[s]
    start = me * span
    group = 256
    heads = group // HEAD_DIM
    own = iota((heads * width, group), 0) // width == iota((heads * width, group), 1) // HEAD_DIM
    scores = []
    for c in range(0, total, group):
        q = q_ref[:, c : c + group].astype(F32)
        diagonal = jnp.where(own, jnp.concatenate([q] * heads, axis=0), 0.0).astype(BF16)
        scores.append(dot_t(diagonal, ck_ref[0, :, c : c + group]))
    score = jnp.concatenate(scores, axis=0) * (HEAD_DIM ** (-0.5)) + bias_ref[...]
    live = start + iota(score.shape, 1) < valid
    stay = soft_stay(score)
    taken = score + stay
    stay = jnp.where(live, stay, 0.0)
    tri = jnp.where(iota((span, span), 0) > iota((span, span), 1), 1.0, 0.0).astype(BF16)
    tail = exact_dot(stay, tri)
    weight = jnp.where(live, jnp.exp(taken + tail), 0.0).astype(BF16)
    logs = jnp.sum(stay, axis=1, keepdims=True)
    at = pl.multiple_of(s * width, width)
    for g, c in enumerate(range(0, total, group)):
        r = slice(g * heads * width, (g + 1) * heads * width)
        full = jnp.where(own, dot(weight[r], cv_ref[0, :, c : c + group]), 0.0)
        log_full = jnp.where(own, logs[r], 0.0)
        block = full[0:width]
        log_block = log_full[0:width]
        for h in range(1, heads):
            block = block + full[h * width : (h + 1) * width]
            log_block = log_block + log_full[h * width : (h + 1) * width]
        for p in range(c // w, (c + group) // w):
            lanes = slice(p * w - c, (p + 1) * w - c)
            pay_ref[p, pl.ds(at, width), :] = block[:, lanes]
            slot = jnp.bitwise_and(iota((8, w), 1), HEAD_DIM - 1) >> 3
            packed = jnp.where(s == 0, jnp.zeros((8, w), F32), pay_ref[p, rows : rows + 8, :])
            for j in range(width // 8):
                packed = jnp.where(
                    slot == s * (width // 8) + j, log_block[8 * j : 8 * j + 8, lanes], packed
                )
            pay_ref[p, rows : rows + 8, :] = packed
    uk_ref[...] = ck_ref[...]
    uv_ref[...] = cv_ref[...]

    @pl.when((valid + width > start) & (valid < start + span))
    def _():
        offset = start + iota((span, width), 0) - valid
        chooser = jnp.where(offset == iota((span, width), 1), 1.0, 0.0).astype(BF16)
        offset = start + iota((span, total), 0) - valid
        inside = (offset >= 0) & (offset < width)
        for fresh, old, out in ((k_ref, ck_ref, uk_ref), (v_ref, cv_ref, uv_ref)):
            placed = dot(chooser, fresh[...])
            out[0] = jnp.where(inside, placed, old[0].astype(F32)).astype(BF16)


def output_kernel(
    n,
    pay_ref,
    tree_sum_ref,
    tree_exp_ref,
    wo_hbm,
    out_ref,
    wo,
    recv,
    att,
    gath,
    wide,
    part,
    other,
    sq,
    sqs,
    load_sem,
    send_sem,
    recv_sem,
    gsend_sem,
    grecv_sem,
    pair_sem,
    ssend_sem,
    srecv_sem,
):
    me = lax.axis_index("kv")
    core = lax.axis_index("tp")
    cores = lax.axis_size("tp")
    load = pltpu.make_async_copy(wo_hbm, wo, load_sem)
    load.start()
    peers = [lax.rem(me + d, n) for d in range(1, n)]
    partners = [lax.rem(core + d, cores) for d in range(1, cores)]
    greet([{"kv": p} for p in peers] + [{"tp": t} for t in partners])

    def push(src, dst, ssem, rsem, p):
        return pltpu.make_async_remote_copy(
            src_ref=src,
            dst_ref=dst.at[me],
            send_sem=ssem.at[p],
            recv_sem=rsem.at[me],
            device_id={"kv": p},
            device_id_type=MESH,
        )

    def arrived(dst, ssem, rsem, p):
        pltpu.make_async_remote_copy(
            src_ref=dst.at[p],
            dst_ref=dst.at[p],
            send_sem=ssem.at[p],
            recv_sem=rsem.at[p],
            device_id={"kv": p},
            device_id_type=MESH,
        ).wait_recv()

    for p in peers:
        push(pay_ref.at[p], recv, send_sem, recv_sem, p).start()
    recv[me] = pay_ref[me]
    rows, w = att.shape
    for p in peers:
        arrived(recv, send_sem, recv_sem, p)
    later = jnp.zeros((8, w), F32)
    scales = [None] * n
    for b in range(n - 1, -1, -1):
        scales[b] = spread(jnp.exp(later), rows)
        later = later + recv[b, rows : rows + 8, :]
    same = iota((w, w), 0) // HEAD_DIM == iota((w, w), 1) // HEAD_DIM
    same = jnp.where(same, 1.0, 0.0).astype(BF16)
    scale = exact_dot(jnp.concatenate(scales, axis=0), same)
    cache_part = jnp.zeros((rows, w), F32)
    for b in range(n):
        cache_part = cache_part + scale[b * rows : (b + 1) * rows] * recv[b, 0:rows, :]
    attended = tree_sum_ref[...] + tree_exp_ref[...] * cache_part
    att[...] = attended.astype(BF16)
    for p in peers:
        push(att, gath, gsend_sem, grecv_sem, p).start()
    gath[me] = att[...]
    load.wait()
    for p in range(n):

        @pl.when(p != me)
        def _():
            arrived(gath, gsend_sem, grecv_sem, p)

        wide[:, p * w : (p + 1) * w] = gath[p]
    part[...] = dot(wide[...], wo[...])
    swaps = [
        pltpu.make_async_remote_copy(
            src_ref=part,
            dst_ref=other.at[d],
            send_sem=pair_sem.at[0, d],
            recv_sem=pair_sem.at[1, d],
            device_id={"tp": t},
            device_id_type=MESH,
        )
        for d, t in enumerate(partners)
    ]
    for swap in swaps:
        swap.start()
    mix = part[...]
    for d, swap in enumerate(swaps):
        swap.wait_recv()
        mix = mix + other[d]
    squares = jnp.sum(mix * mix, axis=1, keepdims=True)
    sq[...] = pack(jnp.broadcast_to(squares, (rows, 128)))
    for p in peers:
        push(sq, sqs, ssend_sem, srecv_sem, p).start()
    sqs[me] = sq[...]
    for p in peers:
        arrived(sqs, ssend_sem, srecv_sem, p)
    total = sqs[0]
    for b in range(1, n):
        total = total + sqs[b]
    inv = lax.rsqrt(unpack_column(total, rows) / D + epsilon)
    out_ref[...] = (mix * inv).astype(BF16)
    for p in peers:
        push(pay_ref.at[p], recv, send_sem, recv_sem, p).wait_send()
        push(att, gath, gsend_sem, grecv_sem, p).wait_send()
        push(sq, sqs, ssend_sem, srecv_sem, p).wait_send()
    for swap in swaps:
        swap.wait_send()


def shards(
    n,
    tokens,
    norm_gain,
    w_query,
    w_key,
    w_value,
    query_gain,
    key_gain,
    head_bias,
    w_output,
    cache_keys,
    cache_values,
    base_length,
    accepted,
    parents,
):
    rows, depth = tokens.shape
    total = w_query.shape[1]
    w = total // n
    heads = w // HEAD_DIM
    seqs, width = parents.shape
    span = cache_keys.shape[1]
    columns = w_output.shape[1]
    vmem = pl.BlockSpec(memory_space=pltpu.VMEM)
    smem = pl.BlockSpec(memory_space=pltpu.SMEM)
    hbm = pl.BlockSpec(memory_space=pl.ANY)
    dma = pltpu.SemaphoreType.DMA
    mine_at = lax.axis_index("kv") * heads
    my_bias = lax.dynamic_slice(head_bias, (mine_at,), (heads,)).reshape(1, heads)
    queries, new_keys, new_values, tree_sum, tree_exp = pl.pallas_call(
        functools.partial(project_kernel, n, width),
        name="project",
        out_shape=[jax.ShapeDtypeStruct((rows, total), BF16)] * 3
        + [jax.ShapeDtypeStruct((rows, w), F32)] * 2,
        in_specs=[vmem, vmem, hbm, hbm, hbm, vmem, vmem, vmem, vmem],
        out_specs=[vmem] * 5,
        scratch_shapes=[
            pltpu.VMEM((depth, total), BF16),
            pltpu.VMEM((depth, total), BF16),
            pltpu.VMEM((depth, total), BF16),
            pltpu.VMEM((n, 3 * rows + 8, w), F32),
            pltpu.VMEM((n // 2, 3 * rows + 8, w), F32),
            pltpu.VMEM((n // 2, 3 * rows + 8, w), F32),
            pltpu.VMEM((n // 2, 3 * rows + 8, w), F32),
            pltpu.VMEM((3 * rows, w), BF16),
            pltpu.VMEM((n, 3 * rows, w), BF16),
            dma((3,)),
            dma((n // 2,)),
            dma((n // 2,)),
            dma((n // 2,)),
            dma((n // 2,)),
            dma((n,)),
            dma((n,)),
        ],
        compiler_params=pltpu.CompilerParams(
            collective_id=0, has_side_effects=True, vmem_limit_bytes=62 * 2**20
        ),
    )(
        tokens,
        norm_gain.reshape(1, depth),
        w_query,
        w_key,
        w_value,
        jnp.tile(query_gain, heads).reshape(1, w),
        jnp.tile(key_gain, heads).reshape(1, w),
        my_bias,
        parents.reshape(rows, 1),
    )
    block = pl.BlockSpec((1, span, total), lambda s: (s, 0, 0))
    fresh = pl.BlockSpec((width, total), lambda s: (s, 0))
    pay, updated_keys, updated_values = pl.pallas_call(
        functools.partial(cache_kernel, n, width),
        name="cache",
        grid=(seqs,),
        out_shape=[
            jax.ShapeDtypeStruct((n, rows + 8, w), F32),
            jax.ShapeDtypeStruct(cache_keys.shape, BF16),
            jax.ShapeDtypeStruct(cache_values.shape, BF16),
        ],
        in_specs=[
            smem,
            smem,
            pl.BlockSpec((total // HEAD_DIM * width, 1), lambda s: (0, 0)),
            fresh,
            fresh,
            fresh,
            block,
            block,
        ],
        out_specs=[pl.BlockSpec((n, rows + 8, w), lambda s: (0, 0, 0)), block, block],
        compiler_params=pltpu.CompilerParams(
            dimension_semantics=("arbitrary",), vmem_limit_bytes=32 * 2**20
        ),
    )(
        base_length,
        accepted,
        jnp.repeat(head_bias, width).reshape(-1, 1),
        queries,
        new_keys,
        new_values,
        cache_keys,
        cache_values,
    )
    layer_out = pl.pallas_call(
        functools.partial(output_kernel, n),
        name="output",
        out_shape=jax.ShapeDtypeStruct((rows, columns), BF16),
        in_specs=[vmem, vmem, vmem, hbm],
        out_specs=vmem,
        scratch_shapes=[
            pltpu.VMEM(w_output.shape, BF16),
            pltpu.VMEM((n, rows + 8, w), F32),
            pltpu.VMEM((rows, w), BF16),
            pltpu.VMEM((n, rows, w), BF16),
            pltpu.VMEM((rows, total), BF16),
            pltpu.VMEM((rows, columns), F32),
            pltpu.VMEM((1, rows, columns), F32),
            pltpu.VMEM((8, 128), F32),
            pltpu.VMEM((n, 8, 128), F32),
            dma,
            dma((n,)),
            dma((n,)),
            dma((n,)),
            dma((n,)),
            dma((2, 1)),
            dma((n,)),
            dma((n,)),
        ],
        compiler_params=pltpu.CompilerParams(
            collective_id=1, has_side_effects=True, vmem_limit_bytes=32 * 2**20
        ),
    )(pay, tree_sum, tree_exp, w_output)
    return layer_out, updated_keys, updated_values


def solution(mesh):
    return jax.shard_map(
        functools.partial(shards, mesh.shape["kv"]),
        mesh=mesh,
        in_specs=(
            P("dp", "kv"),
            P("kv"),
            P("kv", "tp"),
            P("kv", "tp"),
            P("kv", "tp"),
            P(),
            P(),
            P("tp"),
            P("tp", "kv"),
            P("dp", "kv", "tp"),
            P("dp", "kv", "tp"),
            P("dp"),
            P("dp"),
            P("dp", None),
        ),
        out_specs=(P("dp", "kv"), P("dp", "kv", "tp"), P("dp", "kv", "tp")),
        check_vma=False,
    )
```
